32 devices in a mesh: ep: 8 (over z, x), tp: 4 (over y, core).
Axes of the slice: x: 2, y: 2, z: 4, core: 2. Of those that a mesh axis runs over, the one named last changes fastest.
Arguments:
- mix_bgate: bfloat16 [2048, 1024], P('ep', 'tp'), may hold values from -6 to 6
- mix_cgate: bfloat16 [2048, 1024], P('ep', 'tp'), may hold values from -6 to 6
- mix_input: bfloat16 [2048, 1024], P('ep', 'tp'), may hold values from -6 to 6
- conv_taps: float32 [3, 1024], P(None, 'tp'), may hold values from -3.5 to 3.5
- mix_out_w: bfloat16 [1024, 2048], P('tp'), may hold values from -0.1875 to 0.1875
- moe_x: bfloat16 [2048, 2048], P('ep', 'tp'), may hold values from -6 to 6
- moe_gain: float32 [2048], replicated, may hold values from 0.1 to 1.9
- routes: int32 [2048, 2], P('ep'), may hold values from 0 to 7, all different within a row; in each aligned block of 256 rows (0 to 255, 256 to 511, ...) at most 96 rows name the same one
- route_w: float32 [2048, 2], P('ep'), may hold values from 0.2 to 1
- w_gate: bfloat16 [8, 2048, 3584], P('ep', None, 'tp'), may hold values from -0.125 to 0.125
- w_up: bfloat16 [8, 2048, 3584], P('ep', None, 'tp'), may hold values from -0.125 to 0.125
- w_down: bfloat16 [8, 3584, 2048], P('ep', 'tp'), may hold values from -0.09375 to 0.09375
Outputs:
- mixed: bfloat16 [2048, 2048], P(('ep', 'tp'))
- routed: bfloat16 [2048, 2048], P('ep', 'tp')
The draws below stay inside these ranges and needn't reach their ends.
Inputs may be any that keep to these rules, and one draw needn't show every extreme that they name: `routes`: among the 256 rows of one index of ep, each row names 2 different experts and no expert is named by more than 96 rows; in every draw some expert is named by exactly 96 rows of some index.
All inputs are finite; a program needn't handle non-finite values.
Results may differ from the reference program's by a relative error of at most 0.012.
Values may be sent and summed in bfloat16 or wider, within the bound.
No kernel may reach another device: no remote copies, remote signals or barrier semaphores. Data moves between devices by JAX's collectives and lax.ppermute only.
A program may use at most 64 MiB of HBM per device.

```python
import math
import jax
import jax.numpy as jnp
import numpy as np
from jax import lax

D = 2048
CONV = 1024
TAPS = 3
FF_E = 3584
TOPK = 2
TOK_MOE = 256
SEQ = 2048
MOE_TOKENS = 2048
EXPERTS = 8
CAP = 96
N_EP = 8
N_TP = 4


def steps_of(stream_key, shape, split, low, top_value):
    def one(position, shards_of):
        steps = jax.random.uniform(jax.random.fold_in(jax.random.fold_in(stream_key, 6), position), (shards_of,), jnp.float32, low / len(split), top_value / len(split))
        return jnp.repeat(jnp.exp(steps), shape[position] // shards_of).reshape((-1,) + (1,) * (len(shape) - position - 1))

    loudness = one(*split[0])
    for cut in split[1:]:
        loudness = loudness * one(*cut)
    return loudness


def assign_block(own_key, own, number, rows, amount, top, bound, skew):
    sequence = jax.random.permutation(own_key, amount)
    heavy_load, ordinary = portions_of(amount, rows * top, bound, skew, True), portions_of(amount, rows * top, bound, skew, False)
    places = jnp.arange(amount)

    def named(lengths, offset_by):
        used = int((lengths > 0).sum())
        fixed = max(1, used // 4)
        moved = fixed + (places - fixed + offset_by * (used - fixed)) % max(1, amount - fixed)
        return jnp.zeros((amount,), jnp.int32).at[sequence[jnp.where(places < fixed, places, moved)]].set(jnp.asarray(lengths, jnp.int32))

    lengths = jnp.where(number % 4 == 0, named(heavy_load, number // 4), named(ordinary, number - number // 4 - 1))
    mixed = jax.random.permutation(jax.random.fold_in(own, 3), amount)
    source_of, taker = mixed[0:amount // 2 * 2:2], mixed[1:amount // 2 * 2:2]
    slack = jnp.minimum(lengths[source_of] - 1, bound - lengths[taker]) // 2
    slack = jnp.where((source_of == sequence[0]) | (taker == sequence[0]) | (lengths[taker] == 0), 0, jnp.maximum(slack, 0))
    moved = jax.random.randint(jax.random.fold_in(own, 4), (amount // 2,), 0, 1 << 20) % (slack + 1)
    lengths = lengths.at[source_of].add(-moved).at[taker].add(moved)
    items = jnp.searchsorted(jnp.cumsum(lengths), jnp.arange(rows * top), side="right").astype(jnp.int32)
    listing = items.reshape(top, rows).T
    listing = listing[jax.random.permutation(jax.random.fold_in(own, 1), rows)]
    offset_by = jax.random.randint(jax.random.fold_in(own, 2), (rows, 1), 0, top)
    return jnp.take_along_axis(listing, (jnp.arange(top)[None, :] + offset_by) % top, axis=1)


def portions_of(amount, total, reach, lean, full):
    loads = [(1 << 20) // math.isqrt(grade ** lean) + 1 for grade in range(1, amount + 1)]
    largest = reach if full else min(reach, max(-(-total // amount), total * loads[0] // sum(loads)))
    least = 1 if total - largest >= amount - 1 else 0
    counts, surplus = [largest] + [least] * (amount - 1), total - largest - least * (amount - 1)
    while surplus > 0:
        candidates = [i for i in range(1, amount) if counts[i] < largest] or [i for i in range(1, amount) if counts[i] < reach]
        pool, budget = sum([loads[i] for i in candidates]), surplus
        for i in candidates:
            more = min(reach - counts[i], max(1, budget * loads[i] // pool), surplus)
            counts[i] = counts[i] + more
            surplus = surplus - more
    return np.array(counts)


def normal_values(rng, extent, spread, reach, shards=(), kind=jnp.bfloat16):
    factor_of = steps_of(rng, extent, shards, -0.22, 0.18) if shards else 1.0
    array = jax.random.normal(rng, extent, jnp.float32) * spread * factor_of
    return jnp.minimum(jnp.maximum(array, -reach), reach).astype(kind)


def setup_inputs(seed: int = 0) -> dict:
    key_of = jax.random.split(jax.random.key(seed), 13)
    mix_bgate = normal_values(key_of[0], (SEQ, CONV), 1.0, 6.0, ((0, 8), (1, 4)))
    mix_cgate = normal_values(key_of[1], (SEQ, CONV), 1.0, 6.0, ((0, 8), (1, 4)))
    mix_input = normal_values(key_of[2], (SEQ, CONV), 1.0, 6.0, ((0, 8), (1, 4)))
    conv_taps = normal_values(key_of[3], (TAPS, CONV), TAPS ** -0.5, 3.5, ((1, 4),), jnp.float32)
    mix_out_w = normal_values(key_of[4], (CONV, D), CONV ** -0.5, 0.1875, ((0, 4),))
    moe_x = normal_values(key_of[5], (MOE_TOKENS, D), 1.0, 6.0, ((0, 8), (1, 4)))
    moe_gain = jnp.clip(1.0 + 0.18 * jax.random.normal(key_of[6], (D,), jnp.float32), 0.1, 1.9)
    routes_keys = jax.random.split(jax.random.fold_in(key_of[7], 1), MOE_TOKENS // TOK_MOE)
    routes_turns = jax.random.permutation(jax.random.fold_in(key_of[7], 3), MOE_TOKENS // TOK_MOE)
    routes = jax.vmap(lambda own, number: assign_block(jax.random.fold_in(key_of[7], 2), own, number, TOK_MOE, EXPERTS, TOPK, CAP, 2))(routes_keys, routes_turns).reshape((MOE_TOKENS, TOPK))
    route_w = jnp.clip(0.2 + 0.8 * jax.random.uniform(key_of[8], (MOE_TOKENS, TOPK), jnp.float32) ** steps_of(key_of[8], (MOE_TOKENS, TOPK), ((0, 8),), -0.2, 0.2), 0.2, 1.0)
    w_gate = normal_values(key_of[9], (EXPERTS, D, FF_E), D ** -0.5, 0.125, ((0, 8), (2, 4)))
    w_up = normal_values(key_of[10], (EXPERTS, D, FF_E), D ** -0.5, 0.125, ((0, 8), (2, 4)))
    w_down = normal_values(key_of[11], (EXPERTS, FF_E, D), FF_E ** -0.5, 0.09375, ((0, 8), (1, 4)))
    return {"mix_bgate": mix_bgate, "mix_cgate": mix_cgate, "mix_input": mix_input, "conv_taps": conv_taps, "mix_out_w": mix_out_w, "moe_x": moe_x, "moe_gain": moe_gain, "routes": routes, "route_w": route_w, "w_gate": w_gate, "w_up": w_up, "w_down": w_down}


def rms_rows(values, gain):
    wide = values.astype(jnp.float32)
    scale = lax.rsqrt(lax.optimization_barrier(jnp.mean(wide * wide, axis=-1, keepdims=True)) + 1e-06)
    return (wide * scale * gain).astype(jnp.bfloat16)

def rounded(value):
    return lax.optimization_barrier(value.astype(jnp.bfloat16)).astype(jnp.float32)

def reference(mix_bgate, mix_cgate, mix_input, conv_taps, mix_out_w, moe_x, moe_gain, routes, route_w, w_gate, w_up, w_down):
    length = mix_input.shape[0]
    prod = mix_cgate.astype(jnp.float32) * mix_input.astype(jnp.float32)
    padded = jnp.pad(prod, ((TAPS - 1, 0), (0, 0)))
    conv = conv_taps[0] * padded[0:length]
    for j in range(1, TAPS):
        conv = conv + conv_taps[j] * padded[j:j + length]
    gated = (mix_bgate.astype(jnp.float32) * conv).astype(jnp.bfloat16)
    step = CONV // N_TP
    total = jnp.zeros((length, D), jnp.float32)
    for q in range(N_TP):
        part = jnp.dot(gated[:, q * step:(q + 1) * step], mix_out_w[q * step:(q + 1) * step], preferred_element_type=jnp.float32)
        total = total + rounded(part)
    mixed = total.astype(jnp.bfloat16)
    normed = rms_rows(moe_x, moe_gain)
    dev_routes = routes.reshape(N_EP, TOK_MOE * TOPK)
    onehot = (dev_routes[:, :, None] == jnp.arange(EXPERTS, dtype=jnp.int32)[None, None, :]).astype(jnp.int32)
    earlier = jnp.cumsum(onehot, axis=1) - onehot
    slot = lax.optimization_barrier(jnp.sum(earlier * onehot, axis=2))
    row = jnp.arange(N_EP, dtype=jnp.int32)[:, None] * CAP + slot
    flat_e = dev_routes.reshape(-1)
    flat_row = row.reshape(-1).astype(jnp.int32)
    token = jnp.arange(MOE_TOKENS * TOPK, dtype=jnp.int32) // TOPK
    buffers = jnp.zeros((EXPERTS, N_EP * CAP, D), jnp.bfloat16).at[flat_e, flat_row].set(normed[token])
    fstep = FF_E // N_TP

    def expert(items):
        rows, wg, wu, wd = items
        gate = jnp.dot(rows, wg, preferred_element_type=jnp.float32)
        upper = jnp.dot(rows, wu, preferred_element_type=jnp.float32)
        hidden = (jax.nn.silu(gate) * upper).astype(jnp.bfloat16)
        acc = jnp.zeros((rows.shape[0], D), jnp.float32)
        for q in range(N_TP):
            part = jnp.dot(hidden[:, q * fstep:(q + 1) * fstep], wd[q * fstep:(q + 1) * fstep], preferred_element_type=jnp.float32)
            acc = acc + rounded(part)
        return acc.astype(jnp.bfloat16)
    results = lax.map(expert, (buffers, w_gate, w_up, w_down))
    picked = results[flat_e, flat_row].astype(jnp.float32).reshape(MOE_TOKENS, TOPK, D)
    routed = lax.optimization_barrier(jnp.sum(picked * route_w[:, :, None], axis=1)).astype(jnp.bfloat16)
    return (mixed, routed)
```

```python
import functools

import jax
import jax.numpy as jnp
from jax import lax
from jax.experimental import pallas as pl
from jax.experimental.pallas import tpu as pltpu
from jax.sharding import PartitionSpec as P


F32 = jnp.float32
BF16 = jnp.bfloat16
VMEM = pl.BlockSpec(memory_space=pltpu.VMEM)
SMEM = pl.BlockSpec(memory_space=pltpu.SMEM)
ANY = pl.BlockSpec(memory_space=pl.ANY)


def swap(block, axis, bit):
    n = lax.axis_size(axis)
    return lax.ppermute(block, axis, [(i, i ^ bit) for i in range(n)])


def shifted(block, axis, distance):
    devices = range(lax.axis_size(axis))
    route = [(i - distance, i) for i in devices if i - distance in devices]
    return lax.ppermute(block, axis, route)


def bits_of(n):
    return [1 << k for k in range(n.bit_length() - 1)]


def gather_pieces(own):
    pieces = {0: own}
    for bit in reversed(bits_of(lax.axis_size("tp"))):
        for r in list(pieces):
            pieces[r ^ bit] = swap(pieces[r], "tp", bit)
    return [pieces[r] for r in range(len(pieces))]


def reduce_pieces(pieces):
    live = {r: [piece] for r, piece in enumerate(pieces)}

    def total(terms):
        out = terms[0].astype(F32)
        for term in terms[1:]:
            out = out + term.astype(F32)
        return out

    for bit in bits_of(len(pieces)):
        for r in [r for r in reversed(sorted(live)) if r & bit]:
            sent = total(live.pop(r)).astype(BF16)
            live[r ^ bit].append(swap(sent, "tp", bit))
    return total(live[0])


def mixer_kernel(n_tp, me_ref, b_ref, c_ref, x_ref, halo_ref, taps_ref, w_ref, *outs):
    gated_ref = outs[-1]
    outs = outs[:-1]
    length = x_ref.shape[0]
    reach = taps_ref.shape[0] - 1
    prod = c_ref[...].astype(F32) * x_ref[...].astype(F32)
    before = halo_ref[0].astype(F32) * halo_ref[1].astype(F32)
    row = lax.broadcasted_iota(jnp.int32, prod.shape, 0)
    conv = taps_ref[reach : reach + 1, :] * prod
    for back in range(1, reach + 1):
        moved = pltpu.roll(prod, back, 0)
        for r in range(back):
            k = reach - back + r
            moved = jnp.where(row == r, before[k : k + 1, :], moved)
        conv = conv + taps_ref[reach - back : reach - back + 1, :] * moved
    gated_ref[...] = (b_ref[...].astype(F32) * conv).astype(BF16)
    part = length // n_tp
    for r in range(n_tp):
        q = me_ref[0] ^ r
        rows = gated_ref[pl.ds(pl.multiple_of(q * part, part), part), :]
        outs[r][...] = jnp.dot(rows, w_ref[...], preferred_element_type=F32).astype(BF16)


def conv_mixer(tp, mix_bgate, mix_cgate, mix_input, conv_taps, mix_out_w):
    n_tp = lax.axis_size("tp")
    length, chans = mix_input.shape
    width = mix_out_w.shape[1]
    reach = conv_taps.shape[0] - 1
    tail = jnp.stack([mix_cgate[length - reach :], mix_input[length - reach :]])
    halo = shifted(tail, "ep", 1)
    out = jax.ShapeDtypeStruct((length // n_tp, width), BF16)
    pieces = pl.pallas_call(
        functools.partial(mixer_kernel, n_tp),
        out_shape=[out] * n_tp,
        in_specs=[SMEM] + [VMEM] * 6,
        out_specs=[VMEM] * n_tp,
        scratch_shapes=[pltpu.VMEM((length, chans), BF16)],
        compiler_params=pltpu.CompilerParams(vmem_limit_bytes=16 << 20),
        cost_estimate=pl.CostEstimate(
            flops=2 * length * chans * width, bytes_accessed=3 << 20, transcendentals=0
        ),
        name="mixer",
    )(tp, mix_bgate, mix_cgate, mix_input, halo, conv_taps, mix_out_w)
    return reduce_pieces(pieces).astype(BF16)


def places(ep, routes_ref, n_ep):
    rel = routes_ref[...] ^ ep
    top, ntok = rel.shape
    expert = lax.broadcasted_iota(jnp.int32, (n_ep, ntok), 0)
    named = rel[0:1, :] == expert
    for k in range(1, top):
        named = named | (rel[k : k + 1, :] == expert)
    before = lax.broadcasted_iota(jnp.int32, (ntok, ntok), 0) < lax.broadcasted_iota(
        jnp.int32, (ntok, ntok), 1
    )
    slot = jnp.dot(
        named.astype(F32).astype(BF16),
        before.astype(F32).astype(BF16),
        preferred_element_type=F32,
    )
    return jnp.where(named, slot, -1.0)


def dispatch_kernel(n_ep, cap, ep_ref, routes_ref, x_ref, *outs):
    slot = places(ep_ref[0], routes_ref, n_ep)
    ntok = x_ref.shape[0]
    rows = lax.broadcasted_iota(jnp.int32, (cap, ntok), 0).astype(F32)
    for b in range(n_ep):
        pick = (rows == slot[b : b + 1, :]).astype(F32).astype(BF16)
        outs[b][...] = jnp.dot(pick, x_ref[...], preferred_element_type=F32).astype(BF16)


def combine_kernel(n_ep, cap, ep_ref, routes_ref, weight_ref, *refs):
    blocks, out_ref = refs[:-1], refs[-1]
    slot = places(ep_ref[0], routes_ref, n_ep)
    rel = routes_ref[...] ^ ep_ref[0]
    top, ntok = rel.shape
    rows = lax.broadcasted_iota(jnp.int32, (cap, ntok), 0).astype(F32)
    total = jnp.zeros(out_ref.shape, F32)
    contract = (((0,), (0,)), ((), ()))
    for b in range(n_ep):
        weight = jnp.zeros((1, ntok), F32)
        for k in range(top):
            weight = weight + jnp.where(rel[k : k + 1, :] == b, weight_ref[k : k + 1, :], 0.0)
        spread = jnp.where(rows == slot[b : b + 1, :], weight, 0.0)
        high = spread.astype(BF16)
        low = (spread - high.astype(F32)).astype(BF16)
        block = blocks[b][...]
        total = total + lax.dot_general(high, block, contract, preferred_element_type=F32)
        total = total + lax.dot_general(low, block, contract, preferred_element_type=F32)
    out_ref[...] = total.astype(BF16)


def expert_kernel(n_tp, me_ref, gain_ref, wg_ref, wu_ref, wd_ref, *refs):
    pieces, refs = refs[:n_tp], refs[n_tp:]
    outs, refs = refs[:n_tp], refs[n_tp:]
    wg_v, wu_v, wd_v, gate_v, up_v, sem = refs
    part = pieces[0].shape[1]
    width = part * n_tp
    me = me_ref[0]

    def span(r):
        return pl.ds(pl.multiple_of((me ^ r) * part, part), part)

    copies = []
    for r in range(n_tp):
        copies.append(pltpu.make_async_copy(wg_ref.at[0, span(r), :], wg_v.at[r], sem.at[0, r]))
        copies.append(pltpu.make_async_copy(wu_ref.at[0, span(r), :], wu_v.at[r], sem.at[1, r]))
    for r in range(n_tp):
        copies.append(pltpu.make_async_copy(wd_ref.at[0, :, span(r)], wd_v.at[r], sem.at[2, r]))
    for copy in copies:
        copy.start()
    square = None
    for piece in pieces:
        wide = piece[...].astype(F32)
        term = jnp.sum(wide * wide, axis=1, keepdims=True)
        square = term if square is None else square + term
    scale = lax.rsqrt(square / width + 1e-06)
    for r in range(n_tp):
        normed = (pieces[r][...].astype(F32) * scale * gain_ref[:, span(r)]).astype(BF16)
        copies[2 * r].wait()
        gate = jnp.dot(normed, wg_v[r], preferred_element_type=F32)
        gate_v[...] = gate if r == 0 else gate_v[...] + gate
        copies[2 * r + 1].wait()
        up = jnp.dot(normed, wu_v[r], preferred_element_type=F32)
        up_v[...] = up if r == 0 else up_v[...] + up
    value = gate_v[...]
    hidden = (value / (1.0 + jnp.exp(-value)) * up_v[...]).astype(BF16)
    for k in range(n_tp):
        r = n_tp - 1 - k
        copies[2 * n_tp + r].wait()
        outs[r][...] = jnp.dot(hidden, wd_v[r], preferred_element_type=F32).astype(BF16)


def expert_rows(tp, gain, w_gate, w_up, w_down, pieces):
    n_tp = len(pieces)
    rows, part = pieces[0].shape
    width = part * n_tp
    hidden = w_gate.shape[2]
    out = jax.ShapeDtypeStruct((rows, part), BF16)
    return pl.pallas_call(
        functools.partial(expert_kernel, n_tp),
        out_shape=[out] * n_tp,
        in_specs=[SMEM, VMEM, ANY, ANY, ANY] + [VMEM] * n_tp,
        out_specs=[VMEM] * n_tp,
        scratch_shapes=[
            pltpu.VMEM((n_tp, part, hidden), BF16),
            pltpu.VMEM((n_tp, part, hidden), BF16),
            pltpu.VMEM((n_tp, hidden, part), BF16),
            pltpu.VMEM((rows, hidden), F32),
            pltpu.VMEM((rows, hidden), F32),
            pltpu.SemaphoreType.DMA((3, n_tp)),
        ],
        compiler_params=pltpu.CompilerParams(vmem_limit_bytes=40 << 20),
        cost_estimate=pl.CostEstimate(
            flops=6 * rows * width * hidden,
            bytes_accessed=6 * width * hidden,
            transcendentals=rows * hidden,
        ),
        name="experts",
    )(tp, gain, w_gate, w_up, w_down, *pieces)


GROUPS = 2


def expert_layer(ep, tp, moe_x, moe_gain, routes, route_w, w_gate, w_up, w_down):
    ntok, part = moe_x.shape
    top = routes.shape[1]
    n_ep = lax.axis_size("ep")
    assert w_gate.shape[0] == 1
    cap = 4 * ((3 * ntok * top + 8 * n_ep - 1) // (8 * n_ep))
    routes_t = routes.T
    weight_t = route_w.T
    gain = moe_gain.reshape(1, -1)
    block = jax.ShapeDtypeStruct((cap, part), BF16)
    sent = pl.pallas_call(
        functools.partial(dispatch_kernel, n_ep, cap),
        out_shape=[block] * n_ep,
        in_specs=[SMEM, VMEM, VMEM],
        out_specs=[VMEM] * n_ep,
        compiler_params=pltpu.CompilerParams(vmem_limit_bytes=16 << 20),
        cost_estimate=pl.CostEstimate(
            flops=2 * n_ep * cap * ntok * part, bytes_accessed=1 << 20, transcendentals=0
        ),
        name="dispatch",
    )(ep, routes_t, moe_x)
    landed = [sent[0]] + [swap(sent[b], "ep", b) for b in range(1, n_ep)]
    size = n_ep // GROUPS
    back = []
    for g in range(GROUPS):
        own = jnp.concatenate(landed[g * size : (g + 1) * size], 0)
        results = expert_rows(tp, gain, w_gate, w_up, w_down, gather_pieces(own))
        done = reduce_pieces(results).astype(BF16)
        for j in range(size):
            b = g * size + j
            rows = done[j * cap : (j + 1) * cap]
            back.append(rows if b == 0 else swap(rows, "ep", b))
    return pl.pallas_call(
        functools.partial(combine_kernel, n_ep, cap),
        out_shape=jax.ShapeDtypeStruct((ntok, part), BF16),
        in_specs=[SMEM, VMEM, VMEM] + [VMEM] * n_ep,
        out_specs=VMEM,
        compiler_params=pltpu.CompilerParams(vmem_limit_bytes=16 << 20),
        cost_estimate=pl.CostEstimate(
            flops=4 * n_ep * cap * ntok * part, bytes_accessed=1 << 20, transcendentals=0
        ),
        name="combine",
    )(ep, routes_t, weight_t, *back)


def body(
    mix_bgate,
    mix_cgate,
    mix_input,
    conv_taps,
    mix_out_w,
    moe_x,
    moe_gain,
    routes,
    route_w,
    w_gate,
    w_up,
    w_down,
):
    ep = lax.axis_index("ep").astype(jnp.int32).reshape(1)
    tp = lax.axis_index("tp").astype(jnp.int32).reshape(1)
    mixed = conv_mixer(tp, mix_bgate, mix_cgate, mix_input, conv_taps, mix_out_w)
    routed = expert_layer(ep, tp, moe_x, moe_gain, routes, route_w, w_gate, w_up, w_down)
    return (mixed, routed)


def solution(mesh):
    in_specs = (
        P("ep", "tp"),
        P("ep", "tp"),
        P("ep", "tp"),
        P(None, "tp"),
        P("tp", None),
        P("ep", "tp"),
        P(),
        P("ep", None),
        P("ep", None),
        P("ep", None, "tp"),
        P("ep", None, "tp"),
        P("ep", "tp", None),
    )
    out_specs = (P(("ep", "tp"), None), P("ep", "tp"))
    return jax.shard_map(body, mesh=mesh, in_specs=in_specs, out_specs=out_specs, check_vma=False)
```

```python
import functools

import jax
import jax.numpy as jnp
from jax import lax
from jax.experimental import pallas as pl
from jax.experimental.pallas import tpu as pltpu
from jax.sharding import PartitionSpec as P


F32 = jnp.float32
BF16 = jnp.bfloat16
VMEM = pl.BlockSpec(memory_space=pltpu.VMEM)
SMEM = pl.BlockSpec(memory_space=pltpu.SMEM)
HBM = pl.BlockSpec(memory_space=pltpu.HBM)


def swap(block, bit):
    n = lax.axis_size("tp")
    return lax.ppermute(block, "tp", [(i, i ^ bit) for i in range(n)])


def pair_swap(block, b):
    n_ep, n_tp = lax.axis_size("ep"), lax.axis_size("tp")
    route = [
        (i * n_tp + q, (i ^ (b + (q & 1))) * n_tp + q)
        for i in range(n_ep)
        for q in range(n_tp)
    ]
    return lax.ppermute(block, ("ep", "tp"), route)


def shifted(block, distance):
    devices = range(lax.axis_size("ep"))
    route = [(i - distance, i) for i in devices if i - distance in devices]
    return lax.ppermute(block, "ep", route)


def bits_of(n):
    return [1 << k for k in range(n.bit_length() - 1)]


def total(terms):
    out = terms[0].astype(F32)
    for term in terms[1:]:
        out = out + term.astype(F32)
    return out


def spread_far(own):
    pieces = {0: own}
    for bit in reversed(bits_of(lax.axis_size("tp") // 2)):
        for r in list(pieces):
            pieces[r ^ bit] = swap(pieces[r], 2 * bit)
    return [pieces[r] for r in range(len(pieces))]


def reduce_far(kept, sent):
    live = {}
    for r in reversed(range(len(kept))):
        live[r] = [kept[r], swap(sent[r], 1)]
    for bit in reversed(bits_of(len(kept))):
        for r in [r for r in sorted(live) if r & bit]:
            value = total(live.pop(r)).astype(BF16)
            live[r ^ bit].append(swap(value, 2 * bit))
    return total(live[0]).astype(BF16)


def aligned(start, size):
    return pl.ds(pl.multiple_of(start * size, size), size)


def in_hbm(*arrays):
    return [pltpu.with_memory_space_constraint(a, pltpu.HBM) for a in arrays]


def fetch(pairs, sem):
    copies = [
        pltpu.make_async_copy(src, dst, sem.at[k]) for k, (src, dst) in enumerate(pairs)
    ]
    for copy in copies:
        copy.start()
    return copies


def mixer_kernel(n_tp, me_ref, halo_ref, b_hbm, c_hbm, x_hbm, taps_hbm, w_hbm, *refs):
    outs, refs = refs[:n_tp], refs[n_tp:]
    b_ref, c_ref, x_ref, taps_ref, w_ref, gated_ref, sem = refs
    copies = fetch(
        [(c_hbm, c_ref), (x_hbm, x_ref), (taps_hbm, taps_ref), (b_hbm, b_ref), (w_hbm, w_ref)],
        sem,
    )
    for copy in copies[:-1]:
        copy.wait()
    length = x_ref.shape[0]
    reach = taps_ref.shape[0] - 1
    prod = c_ref[...].astype(F32) * x_ref[...].astype(F32)
    before = halo_ref[0].astype(F32) * halo_ref[1].astype(F32)
    row = lax.broadcasted_iota(jnp.int32, prod.shape, 0)
    conv = taps_ref[reach : reach + 1, :] * prod
    for back in range(1, reach + 1):
        moved = pltpu.roll(prod, back, 0)
        for r in range(back):
            k = reach - back + r
            moved = jnp.where(row == r, before[k : k + 1, :], moved)
        conv = conv + taps_ref[reach - back : reach - back + 1, :] * moved
    gated_ref[...] = (b_ref[...].astype(F32) * conv).astype(BF16)
    part = length // n_tp
    copies[-1].wait()
    for r in range(n_tp):
        rows = gated_ref[aligned(me_ref[2] ^ r, part), :]
        outs[r][...] = jnp.dot(rows, w_ref[...], preferred_element_type=F32).astype(BF16)


def conv_mixer(at, mix_bgate, mix_cgate, mix_input, conv_taps, mix_out_w):
    n_tp = lax.axis_size("tp")
    length, chans = mix_input.shape
    width = mix_out_w.shape[1]
    reach = conv_taps.shape[0] - 1
    tail = jnp.stack([mix_cgate[length - reach :], mix_input[length - reach :]])
    halo = shifted(tail, 1)
    out = jax.ShapeDtypeStruct((length // n_tp, width), BF16)
    pieces = pl.pallas_call(
        functools.partial(mixer_kernel, n_tp),
        out_shape=[out] * n_tp,
        in_specs=[SMEM, VMEM] + [HBM] * 5,
        out_specs=[VMEM] * n_tp,
        scratch_shapes=[
            pltpu.VMEM((length, chans), BF16),
            pltpu.VMEM((length, chans), BF16),
            pltpu.VMEM((length, chans), BF16),
            pltpu.VMEM(conv_taps.shape, F32),
            pltpu.VMEM(mix_out_w.shape, BF16),
            pltpu.VMEM((length, chans), BF16),
            pltpu.SemaphoreType.DMA((5,)),
        ],
        compiler_params=pltpu.CompilerParams(vmem_limit_bytes=16 << 20),
        cost_estimate=pl.CostEstimate(
            flops=2 * length * chans * width, bytes_accessed=3 << 20, transcendentals=0
        ),
        name="mixer",
    )(at, halo, *in_hbm(mix_bgate, mix_cgate, mix_input, conv_taps, mix_out_w))
    near = range(0, n_tp, 2)
    return reduce_far([pieces[r] for r in near], [pieces[r + 1] for r in near])


def dispatch_kernel(n_ep, cap, at_ref, own_hbm, other_ref, routes_hbm, weight_hbm, *refs):
    blocks, refs = refs[: n_ep // 2], refs[n_ep // 2 :]
    slot_out, weight_out, both, routes_ref, weight_ref, sem = refs
    core = at_ref[1]
    part = other_ref.shape[1]
    copies = fetch(
        [
            (routes_hbm, routes_ref),
            (weight_hbm, weight_ref),
            (own_hbm, both.at[:, aligned(core, part)]),
        ],
        sem,
    )
    both[:, aligned(1 - core, part)] = other_ref[...]
    copies[0].wait()
    copies[1].wait()
    rel = routes_ref[...] ^ at_ref[0]
    top, ntok = rel.shape
    expert = 2 * lax.broadcasted_iota(jnp.int32, (n_ep // 2, ntok), 0)
    named = rel[0:1, :] == expert
    weight = jnp.where(named, weight_ref[0:1, :], 0.0)
    for k in range(1, top):
        here = rel[k : k + 1, :] == expert
        weight = weight + jnp.where(here, weight_ref[k : k + 1, :], 0.0)
        named = named | here
    before = lax.broadcasted_iota(jnp.int32, (ntok, ntok), 0) < lax.broadcasted_iota(
        jnp.int32, (ntok, ntok), 1
    )
    slot = jnp.dot(
        named.astype(F32).astype(BF16),
        before.astype(F32).astype(BF16),
        preferred_element_type=F32,
    )
    slot = jnp.where(named, slot, -1.0)
    slot_out[...] = slot
    weight_out[...] = weight
    rows = lax.broadcasted_iota(jnp.int32, (cap, ntok), 0).astype(F32)
    copies[2].wait()
    for j in range(n_ep // 2):
        pick = (rows == slot[j : j + 1, :]).astype(F32).astype(BF16)
        blocks[j][...] = jnp.dot(pick, both[...], preferred_element_type=F32).astype(BF16)


def expert_kernel(n_far, me_ref, gain_ref, wg_ref, wu_ref, wd_ref, *refs):
    own, refs = refs[:n_far], refs[n_far:]
    other, refs = refs[:n_far], refs[n_far:]
    kept, refs = refs[:n_far], refs[n_far:]
    sent, (rows_ref,) = refs[:n_far], refs[n_far:]
    half, part = own[0].shape
    me = me_ref[3]
    scales = []
    for refs in (own, other):
        square = None
        for ref in refs:
            wide = ref[...].astype(F32)
            term = jnp.sum(wide * wide, axis=1, keepdims=True)
            square = term if square is None else square + term
        scales.append(lax.rsqrt(square / (part * n_far) + 1e-06))
    gate = up = None
    for r in range(n_far):
        at = aligned(me ^ r, part)
        for k, ref in enumerate((own[r], other[r])):
            normed = ref[...].astype(F32) * scales[k] * gain_ref[:, at]
            rows_ref[r, k * half : (k + 1) * half, :] = normed.astype(BF16)
        g = jnp.dot(rows_ref[r], wg_ref[0, at, :], preferred_element_type=F32)
        u = jnp.dot(rows_ref[r], wu_ref[0, at, :], preferred_element_type=F32)
        gate = g if gate is None else gate + g
        up = u if up is None else up + u
    hidden = (gate / (1.0 + jnp.exp(-gate)) * up).astype(BF16)
    for r in reversed(range(n_far)):
        at = aligned(me ^ r, part)
        out = jnp.dot(hidden, wd_ref[0, :, at], preferred_element_type=F32).astype(BF16)
        kept[r][...] = out[:half]
        sent[r][...] = out[half:]


def combine_kernel(rows_of, last, at_ref, slot_ref, weight_ref, *refs):
    n = len(rows_of)
    blocks, refs = refs[:n], refs[n:]
    acc = None
    if last:
        before_ref, sent_ref, kept_ref, sum_ref = refs
        acc = before_ref[...]
    else:
        (sum_ref,) = refs
    ntok = sum_ref.shape[0]
    contract = (((0,), (0,)), ((), ()))
    for ref, j in zip(blocks, rows_of):
        rows = lax.broadcasted_iota(jnp.int32, (ref.shape[0], ntok), 0).astype(F32)
        spread = jnp.where(rows == slot_ref[j : j + 1, :], weight_ref[j : j + 1, :], 0.0)
        high = spread.astype(BF16)
        low = (spread - high.astype(F32)).astype(BF16)
        block = ref[...]
        term = lax.dot_general(high, block, contract, preferred_element_type=F32)
        term = term + lax.dot_general(low, block, contract, preferred_element_type=F32)
        acc = term if acc is None else acc + term
    sum_ref[...] = acc
    if last:
        part = kept_ref.shape[1]
        kept_ref[...] = sum_ref[:, aligned(at_ref[1], part)]
        sent_ref[...] = sum_ref[:, aligned(1 - at_ref[1], part)].astype(BF16)


def expert_layer(at, moe_x, moe_gain, routes, route_w, w_gate, w_up, w_down):
    ntok, part = moe_x.shape
    top = routes.shape[1]
    n_ep, n_tp = lax.axis_size("ep"), lax.axis_size("tp")
    n_far = n_tp // 2
    assert w_gate.shape[0] == 1
    cap = 4 * ((3 * ntok * top + 8 * n_ep - 1) // (8 * n_ep))
    gain = moe_gain.reshape(1, -1)
    wide = 2 * part
    n_ops = n_ep // 2
    n_groups = min(4, n_ops)
    per_group = n_ops // n_groups

    other_x = swap(moe_x, 1)
    block = jax.ShapeDtypeStruct((cap, wide), BF16)
    table = jax.ShapeDtypeStruct((n_ops, ntok), F32)
    *sent, slots, weights = pl.pallas_call(
        functools.partial(dispatch_kernel, n_ep, cap),
        out_shape=[block] * n_ops + [table] * 2,
        in_specs=[SMEM, HBM, VMEM, HBM, HBM],
        out_specs=[VMEM] * (n_ops + 2),
        scratch_shapes=[
            pltpu.VMEM((ntok, wide), BF16),
            pltpu.VMEM((top, ntok), jnp.int32),
            pltpu.VMEM((top, ntok), F32),
            pltpu.SemaphoreType.DMA((3,)),
        ],
        compiler_params=pltpu.CompilerParams(vmem_limit_bytes=16 << 20),
        cost_estimate=pl.CostEstimate(
            flops=1 << 36, bytes_accessed=1 << 20, transcendentals=0
        ),
        name="dispatch",
    )(at, *in_hbm(moe_x), other_x, *in_hbm(routes.T, route_w.T))
    stack = [w_gate, w_up, w_down]
    back = {}
    for g in ORDER[n_groups]:
        ops = range(g * per_group, (g + 1) * per_group)
        landed = [pair_swap(sent[j], 2 * j) for j in ops]
        own = landed[0] if per_group == 1 else jnp.concatenate(landed, 0)
        own = spread_far(own)
        other = [swap(own[r], 1) for r in range(n_far)]
        rows = per_group * cap
        out = jax.ShapeDtypeStruct((rows, wide), BF16)
        results = pl.pallas_call(
            functools.partial(expert_kernel, n_far),
            out_shape=[out] * (2 * n_far),
            in_specs=[SMEM] + [VMEM] * (4 + 2 * n_far),
            out_specs=[VMEM] * (2 * n_far),
            scratch_shapes=[pltpu.VMEM((n_far, 2 * rows, wide), BF16)],
            compiler_params=pltpu.CompilerParams(vmem_limit_bytes=24 << 20),
            cost_estimate=pl.CostEstimate(
                flops=12 * rows * wide * n_far * w_gate.shape[2],
                bytes_accessed=8 * rows * wide * n_far,
                transcendentals=2 * rows * w_gate.shape[2],
            ),
            name="experts",
        )(at, gain, *stack, *own, *other)
        done = reduce_far(results[:n_far], results[n_far:])
        for k, j in enumerate(ops):
            back[j] = pair_swap(done[k * cap : (k + 1) * cap], 2 * j)

    def combine(rows_of, before):
        kept = jax.ShapeDtypeStruct((ntok, part), F32)
        crossing = jax.ShapeDtypeStruct((ntok, part), BF16)
        acc = jax.ShapeDtypeStruct((ntok, wide), F32)
        outs = [crossing, kept] if before else [acc]
        return pl.pallas_call(
            functools.partial(combine_kernel, rows_of, bool(before)),
            out_shape=outs,
            in_specs=[SMEM] + [VMEM] * (2 + len(rows_of) + len(before)),
            out_specs=[VMEM] * len(outs),
            scratch_shapes=[pltpu.VMEM(acc.shape, F32)] if before else [],
            compiler_params=pltpu.CompilerParams(vmem_limit_bytes=16 << 20),
            cost_estimate=pl.CostEstimate(
                flops=4 * len(rows_of) * cap * ntok * wide,
                bytes_accessed=1 << 20,
                transcendentals=0,
            ),
            name="combine",
        )(at, slots, weights, *[back[j] for j in rows_of], *before)

    final = ORDER[n_groups][-1]
    late = [j for j in range(n_ops) if j // per_group == final]
    early = [j for j in range(n_ops) if j not in late]
    acc = combine(early, [])
    crossing, kept = combine(late, acc)
    crossed = swap(crossing, 1)
    return (kept + crossed.astype(F32)).astype(BF16)


ORDER = {1: [0], 2: [1, 0], 4: [2, 0, 3, 1]}


def body(
    mix_bgate,
    mix_cgate,
    mix_input,
    conv_taps,
    mix_out_w,
    moe_x,
    moe_gain,
    routes,
    route_w,
    w_gate,
    w_up,
    w_down,
):
    ep = lax.axis_index("ep").astype(jnp.int32)
    tp = lax.axis_index("tp").astype(jnp.int32)
    core = tp & 1
    at = jnp.stack([ep ^ core, core, tp, tp >> 1])
    mixed = conv_mixer(at, mix_bgate, mix_cgate, mix_input, conv_taps, mix_out_w)
    routed = expert_layer(at, moe_x, moe_gain, routes, route_w, w_gate, w_up, w_down)
    return (mixed, routed)


def solution(mesh):
    in_specs = (
        P("ep", "tp"),
        P("ep", "tp"),
        P("ep", "tp"),
        P(None, "tp"),
        P("tp", None),
        P("ep", "tp"),
        P(),
        P("ep", None),
        P("ep", None),
        P("ep", None, "tp"),
        P("ep", None, "tp"),
        P("ep", "tp", None),
    )
    out_specs = (P(("ep", "tp"), None), P("ep", "tp"))
    return jax.shard_map(body, mesh=mesh, in_specs=in_specs, out_specs=out_specs, check_vma=False)
```
